32 devices in a mesh: sp: 8 (over z, x), tp: 4 (over y, core).
Axes of the slice: x: 2, y: 2, z: 4, core: 2. Of those that a mesh axis runs over, the one named last changes fastest.
Arguments:
- queries: bfloat16 [4096, 1024], P('sp', 'tp'), may hold values from -5.5 to 5.5
- key_vectors: bfloat16 [4096, 1024], P('sp', 'tp'), may hold values from -5.5 to 5.5
- latents: bfloat16 [4096, 2048], P('sp', 'tp'), may hold values from -6 to 6
- w_value: bfloat16 [2048, 1024], P(None, 'tp'), may hold values from -0.125 to 0.125
- log_sums: float32 [4096, 16], P('sp', 'tp'), as said below
- out_pair: bfloat16 [4096, 2048], P('sp', 'tp'), may hold values from -6 to 6
- cotangent: bfloat16 [4096, 1024], P('sp', 'tp'), may hold values from -6 to 6
- lambdas: float32 [8], P('tp'), may hold values from 0.3 to 0.8
- out_gain: float32 [128], replicated, may hold values from 0.1 to 1.9
Outputs:
- query_grad: float32 [4096, 1024], P('sp', 'tp')
- key_grad: float32 [4096, 1024], P('sp', 'tp')
- value_grad: float32 [4096, 1024], P('sp', 'tp')
- weight_grad: float32 [2048, 1024], P('sp', 'tp')
The draws below stay inside these ranges and needn't reach their ends.
Inputs may be any that keep to these rules, and one draw needn't show every extreme that they name: `log_sums`: each entry is the logarithm of the sum of exp(scores_c[t, s]) over s <= t for its row t, head h and map c.
All inputs are finite; a program needn't handle non-finite values.
Results may differ from the reference program's by a relative error of at most 0.008.
Values may be sent and summed in bfloat16 or wider, within the bound.
A program may use at most 64 MiB of HBM per device.

```python
import jax
import jax.numpy as jnp
from jax import lax

TOK_DEV = 512
D = 2048
HEADS = 8
QK = 64
VALUE = 128
SEQ = 4096


def pair_draw(key):
    arr_shape = (SEQ, HEADS * 2 * QK)
    key_query = jax.random.fold_in(key, 501)
    key_keys = jax.random.fold_in(key, 502)
    query_vals = jnp.clip(1.3 * jax.random.normal(key_query, arr_shape, jnp.float32), -5.5, 5.5)
    key_vals = jnp.clip(1.3 * jax.random.normal(key_keys, arr_shape, jnp.float32), -5.5, 5.5)
    return (query_vals.astype(jnp.bfloat16), key_vals.astype(jnp.bfloat16))


def draw_queries(key, part):
    return pair_draw(key)[0]


def draw_key_vectors(key, part):
    return pair_draw(key)[1]


def draw_log_sums(key, part):
    query_vals, key_vals = pair_draw(key)
    query_wide = query_vals.astype(jnp.float32).reshape(SEQ, HEADS * 2, QK)
    key_wide = key_vals.astype(jnp.float32).reshape(SEQ, HEADS * 2, QK)
    factor = QK ** (-0.5)
    key_pos = jnp.arange(SEQ, dtype=jnp.int32)

    def per_block(block_idx):
        begin_row = (block_idx * TOK_DEV).astype(jnp.int32)
        query_block = lax.dynamic_slice_in_dim(query_wide, begin_row, TOK_DEV, 0)
        query_pos = begin_row + jnp.arange(TOK_DEV, dtype=jnp.int32)
        visible = key_pos[None, :] <= query_pos[:, None]

        def per_map(map_idx):
            query_map = lax.dynamic_index_in_dim(query_block, map_idx, 1, keepdims=False)
            key_map = lax.dynamic_index_in_dim(key_wide, map_idx, 1, keepdims=False)
            scores = jnp.dot(query_map, key_map.T, precision=lax.Precision.HIGHEST) * factor
            masked = jnp.where(visible, scores, -jnp.inf)
            largest = jnp.max(masked, axis=1)
            return largest + jnp.log(jnp.sum(jnp.where(visible, jnp.exp(masked - largest[:, None]), 0.0), axis=1))
        return lax.map(per_map, jnp.arange(HEADS * 2, dtype=jnp.int32)).T
    result = lax.map(per_block, jnp.arange(SEQ // TOK_DEV, dtype=jnp.int32))
    return result.reshape(SEQ, HEADS * 2).astype(jnp.float32)


def with_spikes(values, rng, source, target, parts, factor):
    owner, partner = [(jnp.arange(values.shape[axis_at]) // (values.shape[axis_at] // parts)).reshape([-1 if axis == axis_at else 1 for axis in range(values.ndim)]) for axis_at in (source, target)]
    chosen = jax.random.permutation(rng, parts)[partner]
    strong = (owner == chosen) | (owner == (partner + parts // 2) % parts)
    return jnp.where(strong, factor * values, values)


def levels(own_key, extent, split, low, high):
    factor_of, own = 1.0, jax.random.fold_in(own_key, 6)
    for axis_at, shards_of in split:
        steps = jnp.exp(jax.random.uniform(jax.random.fold_in(own, axis_at), (shards_of,), jnp.float32, low / len(split), high / len(split)))
        factor_of = factor_of * jnp.repeat(steps, extent[axis_at] // shards_of).reshape([-1 if axis == axis_at else 1 for axis in range(len(extent))])
    return factor_of


def scatter_about(key, dims, width, bound, split=(), kind=jnp.bfloat16):
    values = width * jax.random.normal(key, dims, jnp.float32)
    if split:
        values = values * levels(key, dims, split, -0.22, 0.18)
    return jnp.clip(values, -bound, bound).astype(kind)


def gaussian_with(rng, extent, deviation, bound, split, heavy, kind=jnp.bfloat16):
    drawn = deviation * jax.random.normal(rng, extent, jnp.float32)
    if split:
        drawn = drawn * levels(rng, extent, split, -0.22, 0.18)
    return jnp.clip(with_spikes(drawn, jax.random.fold_in(rng, 3), *heavy), -bound, bound).astype(kind)


def setup_inputs(seed: int = 0) -> dict:
    keys = jax.random.split(jax.random.key(seed), 10)
    queries = draw_queries(jax.random.fold_in(keys[9], 71), 0)
    key_vectors = draw_key_vectors(jax.random.fold_in(keys[9], 71), 0)
    latents = scatter_about(keys[2], (SEQ, D), 1.0, 6.0, ((0, 8), (1, 4)))
    w_value = scatter_about(keys[3], (D, HEADS * VALUE), D ** -0.5, 0.125, ((1, 4),))
    log_sums = draw_log_sums(jax.random.fold_in(keys[9], 71), 0)
    out_pair = scatter_about(keys[5], (SEQ, HEADS * 2 * VALUE), 1.0, 6.0, ((0, 8), (1, 4)))
    cotangent = gaussian_with(keys[6], (SEQ, HEADS * VALUE), 1.0, 6.0, ((0, 8), (1, 4)), (0, 1, 8, 2.0))
    lambdas = jnp.clip(0.3 + 0.5 * jax.random.uniform(keys[7], (HEADS,), jnp.float32) ** levels(keys[7], (HEADS,), ((0, 4),), -0.2, 0.2), 0.3, 0.8)
    out_gain = jnp.clip(1.0 + 0.18 * jax.random.normal(keys[8], (VALUE,), jnp.float32), 0.1, 1.9)
    return dict(queries=queries, key_vectors=key_vectors, latents=latents, w_value=w_value, log_sums=log_sums, out_pair=out_pair, cotangent=cotangent, lambdas=lambdas, out_gain=out_gain)


norm_floor = 0.25

def head_cotangent(out_pair, cotangent, lambdas, out_gain):
    tok_rows = out_pair.shape[0]
    head_count = lambdas.shape[0]
    out_maps = out_pair.astype(jnp.float32).reshape(tok_rows, head_count, 2, -1)
    lam_cols = lambdas[None, :, None]
    merged = out_maps[:, :, 0] - lam_cols * out_maps[:, :, 1]
    inv_norm = lax.rsqrt(lax.optimization_barrier(jnp.mean(merged * merged, axis=-1, keepdims=True)) + norm_floor)
    scaled = cotangent.astype(jnp.float32).reshape(merged.shape) * out_gain
    inner_dot = lax.optimization_barrier(jnp.mean(scaled * merged, axis=-1, keepdims=True))
    out_grad = (inv_norm * scaled - merged * (inv_norm * inv_norm * inv_norm) * inner_dot).astype(jnp.bfloat16)
    grad_wide = out_grad.astype(jnp.float32)
    first_map = lax.optimization_barrier(jnp.sum(grad_wide * out_maps[:, :, 0], axis=-1))
    second_map = -lambdas[None, :] * lax.optimization_barrier(jnp.sum(grad_wide * out_maps[:, :, 1], axis=-1))
    return (out_grad, jnp.stack([first_map, second_map], axis=-1))

def block_terms(query_block, key_block, value_block, grad_block, log_block, term_block, lambdas, query_pos, key_pos):
    factor = query_block.shape[-1] ** (-0.5)
    scores = jnp.einsum('qhcd,khcd->hcqk', query_block.astype(jnp.float32), key_block.astype(jnp.float32)) * factor
    visible = key_pos[None, :] <= query_pos[:, None]
    shifted = scores - jnp.transpose(log_block, (1, 2, 0))[..., None]
    softmax_maps = jnp.where(visible, jnp.exp(shifted), 0.0)
    value_dot = jnp.einsum('qhe,khe->hqk', grad_block.astype(jnp.float32), value_block.astype(jnp.float32))
    lam_cols = lambdas[:, None, None]
    weights = (softmax_maps[:, 0] - lam_cols * softmax_maps[:, 1]).astype(jnp.bfloat16)
    term_cols = jnp.transpose(term_block, (1, 2, 0))
    first_map = softmax_maps[:, 0] * (value_dot - term_cols[:, 0, :, None])
    second_map = softmax_maps[:, 1] * (-lam_cols * value_dot - term_cols[:, 1, :, None])
    dscore = (jnp.stack([first_map, second_map], axis=1) * factor).astype(jnp.bfloat16)
    return (weights, dscore)

def reference(queries, key_vectors, latents, w_value, log_sums, out_pair, cotangent, lambdas, out_gain):
    values = jnp.dot(latents, w_value, preferred_element_type=jnp.float32).astype(jnp.bfloat16)
    out_grad, row_terms = head_cotangent(out_pair, cotangent, lambdas, out_gain)
    query_heads = jnp.moveaxis(queries.reshape(SEQ, HEADS, 1, 2, QK), 1, 0)
    key_heads = jnp.moveaxis(key_vectors.reshape(SEQ, HEADS, 1, 2, QK), 1, 0)
    value_heads = jnp.moveaxis(values.reshape(SEQ, HEADS, 1, VALUE), 1, 0)
    grad_heads = jnp.moveaxis(out_grad.reshape(SEQ, HEADS, 1, VALUE), 1, 0)
    log_heads = jnp.moveaxis(log_sums.reshape(SEQ, HEADS, 1, 2), 1, 0)
    term_heads = jnp.moveaxis(row_terms.reshape(SEQ, HEADS, 1, 2), 1, 0)
    lam_heads = lambdas.reshape(HEADS, 1)
    key_pos = jnp.arange(SEQ, dtype=jnp.int32)

    def one_head(inputs):
        query_head, key_head, value_head, grad_head, log_head, term_head, lam_head = inputs

        def one_block(partial_value, block_idx):
            begin_row = (block_idx * TOK_DEV).astype(jnp.int32)
            query_block = lax.dynamic_slice_in_dim(query_head, begin_row, TOK_DEV, 0)
            grad_block = lax.dynamic_slice_in_dim(grad_head, begin_row, TOK_DEV, 0)
            log_block = lax.dynamic_slice_in_dim(log_head, begin_row, TOK_DEV, 0)
            term_block = lax.dynamic_slice_in_dim(term_head, begin_row, TOK_DEV, 0)
            query_pos = begin_row + jnp.arange(TOK_DEV, dtype=jnp.int32)
            weights, dscore = block_terms(query_block, key_head, value_head, grad_block, log_block, term_block, lam_head, query_pos, key_pos)
            score_wide = dscore.astype(jnp.float32)
            query_part = jnp.einsum('hcqk,khcd->qhcd', score_wide, key_head.astype(jnp.float32))
            key_part = jnp.einsum('hcqk,qhcd->khcd', score_wide, query_block.astype(jnp.float32))
            value_part = jnp.einsum('hqk,qhe->khe', weights.astype(jnp.float32), grad_block.astype(jnp.float32))
            return ((partial_value[0] + key_part, partial_value[1] + value_part), query_part)
        start_sums = (jnp.zeros(key_head.shape, jnp.float32), jnp.zeros(value_head.shape, jnp.float32))
        sums, query_parts = lax.scan(one_block, start_sums, jnp.arange(SEQ // TOK_DEV, dtype=jnp.int32))
        return (query_parts.reshape(query_head.shape), sums[0], sums[1])
    query_grad, key_grad, value_grad = lax.map(one_head, (query_heads, key_heads, value_heads, grad_heads, log_heads, term_heads, lam_heads))
    query_grad = jnp.moveaxis(query_grad, 0, 1).reshape(SEQ, HEADS * 2 * QK)
    key_grad = jnp.moveaxis(key_grad, 0, 1).reshape(SEQ, HEADS * 2 * QK)
    value_grad = jnp.moveaxis(value_grad, 0, 1).reshape(SEQ, HEADS * VALUE)
    value_narrow = value_grad.astype(jnp.bfloat16)
    weight_grad = jnp.dot(latents.T, value_narrow, preferred_element_type=jnp.float32)
    return (query_grad, key_grad, value_grad, weight_grad)
```

```python
import functools
import math

import jax
import jax.numpy as jnp
from jax import lax
from jax.experimental import pallas as pl
from jax.experimental.pallas import tpu as pltpu
from jax.sharding import PartitionSpec as P

MESH = pl.DeviceIdType.MESH
F32 = jnp.float32
BF16 = jnp.bfloat16
LOG2E = math.log2(math.e)
norm_floor = 0.25
TILE = 256


def dot_nn(a, b):
    return lax.dot_general(a, b, (((1,), (0,)), ((), ())), preferred_element_type=F32)


def dot_nt(a, b):
    return lax.dot_general(a, b, (((1,), (1,)), ((), ())), preferred_element_type=F32)


def dot_tn(a, b):
    return lax.dot_general(a, b, (((0,), (0,)), ((), ())), preferred_element_type=F32)


def halves(block, factor):
    width = block.shape[-1]
    lane = lax.broadcasted_iota(jnp.int32, block.shape, 1)
    wide = block.astype(F32) * factor
    return (
        jnp.where(lane < width // 2, wide, 0.0).astype(BF16),
        jnp.where(lane < width // 2, 0.0, wide).astype(BF16),
    )


def kernel(
    n,
    tp_n,
    q_ref,
    k_ref,
    lat_ref,
    w_ref,
    log_ref,
    pair_ref,
    cot_ref,
    lam_ref,
    gain_ref,
    dq_ref,
    dk_ref,
    dv_ref,
    dw_ref,
    kbuf,
    vbuf,
    qbuf,
    gbuf,
    abuf,
    lbuf,
    own_v,
    own_g,
    own_a,
    col_a,
    own_k2,
    own_q2,
    part,
    wbuf,
    lat_send,
    lat_recv,
    fwd_send,
    fwd_recv,
    k_send,
    k_recv,
    v_send,
    v_recv,
    q_send,
    q_recv,
    g_send,
    g_recv,
    a_send,
    a_recv,
    w_send,
    w_recv,
):
    heads = lam_ref.shape[0]
    rows = q_ref.shape[0]
    width = q_ref.shape[1] // heads
    me = lax.axis_index("sp")
    tp = lax.axis_index("tp")
    chain = n // 2
    pos = me // 2
    col = me % 2
    factor = (width // 2) ** (-0.5)

    barrier = pltpu.get_barrier_semaphore()

    def greet_sp(i, carry):
        @pl.when(i != me)
        def _():
            pl.semaphore_signal(barrier, inc=1, device_id=(i, tp), device_id_type=MESH)

        return carry

    def greet_tp(i, carry):
        @pl.when(i != tp)
        def _():
            pl.semaphore_signal(barrier, inc=1, device_id=(me, i), device_id_type=MESH)

        return carry

    lax.fori_loop(0, n, greet_sp, 0)
    lax.fori_loop(0, tp_n, greet_tp, 0)
    pl.semaphore_wait(barrier, n - 1 + tp_n - 1)

    core = tp % 2
    pair = tp // 2
    mate = 2 * pair + 1 - core
    pairs = tp_n // 2

    def rc(src, dst, ssem, rsem, dev):
        return pltpu.make_async_remote_copy(
            src_ref=src,
            dst_ref=dst,
            send_sem=ssem,
            recv_sem=rsem,
            device_id=dev,
            device_id_type=MESH,
        )

    def lat_copy(slot_src, y):
        return rc(
            lat_ref, lbuf.at[slot_src], lat_send.at[y], lat_recv.at[slot_src], (me, 2 * y + core)
        )

    def lat_mate():
        return rc(lat_ref, lbuf.at[tp], fwd_send.at[tp], fwd_recv.at[tp], (me, mate))

    def lat_fwd(src):
        return rc(lbuf.at[src], lbuf.at[src], fwd_send.at[src], fwd_recv.at[src], (me, mate))

    class Stream:
        def __init__(self, own, buf, ssem, rsem, step):
            self.own, self.buf, self.ssem, self.rsem, self.step = own, buf, ssem, rsem, step

        def onward(self):
            nxt = pos + self.step
            return jnp.logical_and(nxt >= 0, nxt < chain)

        def copies(self, src, ref):
            far = rc(
                ref,
                self.buf.at[src],
                self.ssem.at[0, src],
                self.rsem.at[src],
                (jnp.clip(me + 2 * self.step, 0, n - 1), tp),
            )
            side = rc(
                ref,
                self.buf.at[src],
                self.ssem.at[1, src],
                self.rsem.at[src],
                (2 * pos + 1 - col, tp),
            )
            return far, side

        def send_own(self, act):
            far, side = self.copies(me, self.own)

            @pl.when(self.onward())
            def _():
                getattr(far, act)()

            @pl.when(col == (0 if self.step == 1 else 1))
            def _():
                getattr(side, act)()

        def forward(self, src, act):
            far, side = self.copies(src, self.buf.at[src])
            getattr(side, act)()

            @pl.when(self.onward())
            def _():
                getattr(far, act)()

        def wait(self, src):
            self.copies(src, self.buf.at[src])[0].wait_recv()

    ks = Stream(k_ref, kbuf, k_send, k_recv, 1)
    vs = Stream(own_v, vbuf, v_send, v_recv, 1)
    qs = Stream(q_ref, qbuf, q_send, q_recv, -1)
    gs = Stream(own_g, gbuf, g_send, g_recv, -1)
    as_ = Stream(own_a, abuf, a_send, a_recv, -1)

    for y in range(pairs):

        @pl.when(y != pair)
        def _():
            lat_copy(tp, y).start()

    lat_mate().start()
    qs.send_own("start")
    ks.send_own("start")

    lane = lax.broadcasted_iota(jnp.int32, (rows, 128), 1)
    packed = jnp.zeros((rows, 128), F32)
    for h in range(heads):
        lam = lam_ref[h]
        a = pair_ref[:, (2 * h) * width : (2 * h + 1) * width].astype(F32)
        b = pair_ref[:, (2 * h + 1) * width : (2 * h + 2) * width].astype(F32)
        merged = a - lam * b
        inv = lax.rsqrt(jnp.mean(merged * merged, axis=-1, keepdims=True) + norm_floor)
        g = cot_ref[:, h * width : (h + 1) * width].astype(F32) * gain_ref[...]
        inner = jnp.mean(g * merged, axis=-1, keepdims=True)
        og = (inv * g - merged * (inv * inv * inv) * inner).astype(BF16)
        own_g[:, h * width : (h + 1) * width] = og
        wide = og.astype(F32)
        first = jnp.sum(wide * a, axis=-1, keepdims=True)
        second = jnp.sum(wide * b, axis=-1, keepdims=True)
        log_lam = jnp.log(jnp.full((1, 128), lam, F32))
        log0 = log_ref[:, 2 * h : 2 * h + 1] * LOG2E
        log1 = (log_ref[:, 2 * h + 1 : 2 * h + 2] - log_lam) * LOG2E
        packed = jnp.where(lane == 4 * h, log0, packed)
        packed = jnp.where(lane == 4 * h + 1, log1, packed)
        packed = jnp.where(lane == 4 * h + 2, first, packed)
        packed = jnp.where(lane == 4 * h + 3, second, packed)
    col_a[...] = packed
    own_a[...] = jnp.transpose(packed)[:8, :]
    gs.send_own("start")
    as_.send_own("start")

    for h in range(heads):
        sl = slice(h * width, (h + 1) * width)
        k0, k1 = halves(k_ref[:, sl], factor)
        own_k2[0, :, sl] = k0
        own_k2[1, :, sl] = k1
        q0, q1 = halves(q_ref[:, sl], factor)
        own_q2[0, :, sl] = q0
        own_q2[1, :, sl] = q1

    for y in range(pairs):

        @pl.when(y != pair)
        def _():
            src = 2 * y + core
            lat_copy(src, y).wait_recv()
            lat_fwd(src).start()

    local = w_ref.shape[0] // tp_n
    lat_own = pl.ds(pl.multiple_of(tp * local, local), local)
    dv_ref[...] = dot_nn(lat_ref[...], w_ref[lat_own, :])

    for y in range(pairs):
        other = 2 * y + 1 - core
        lat_fwd(other).wait_recv()

    def add_values(i, carry):
        @pl.when(i != tp)
        def _():
            dv_ref[...] += dot_nn(
                lbuf[i], w_ref[pl.ds(pl.multiple_of(i * local, local), local), :]
            )

        return carry

    lax.fori_loop(0, tp_n, add_values, 0)
    own_v[...] = dv_ref[...].astype(BF16)
    vs.send_own("start")

    def key_side(q_of, g_of, a_of, diagonal):
        for h in range(heads):
            sl = slice(h * width, (h + 1) * width)

            def tile(i, carry):
                ts = pl.ds(pl.multiple_of(i * TILE, TILE), TILE)
                q = q_of(sl)
                g = g_of(sl)
                q0, q1 = halves(q, factor)
                s0 = dot_nt(own_k2[0, ts, sl], q)
                s1 = dot_nt(own_k2[1, ts, sl], q)
                vd = dot_nt(own_v[ts, sl], g)
                p0 = jnp.exp2(s0 * LOG2E - a_of(4 * h))
                p1 = jnp.exp2(s1 * LOG2E - a_of(4 * h + 1))
                if diagonal:
                    spos = i * TILE + lax.broadcasted_iota(jnp.int32, (TILE, rows), 0)
                    tpos = lax.broadcasted_iota(jnp.int32, (TILE, rows), 1)
                    vis = spos <= tpos
                    p0 = jnp.where(vis, p0, 0.0)
                    p1 = jnp.where(vis, p1, 0.0)
                mixed = (p0 - p1).astype(BF16)
                d0 = (p0 * (vd - a_of(4 * h + 2))).astype(BF16)
                d1 = (p1 * (a_of(4 * h + 3) - vd)).astype(BF16)
                dvt = dot_nn(mixed, g)
                dkt = dot_nn(d0, q0) + dot_nn(d1, q1)
                if diagonal:
                    dv_ref[ts, sl] = dvt
                    dk_ref[ts, sl] = dkt
                else:
                    dv_ref[ts, sl] += dvt
                    dk_ref[ts, sl] += dkt
                return carry

            lax.fori_loop(0, rows // TILE, tile, 0)

    def query_side(k_of, v_of, diagonal):
        for h in range(heads):
            sl = slice(h * width, (h + 1) * width)

            def tile(i, carry):
                ts = pl.ds(pl.multiple_of(i * TILE, TILE), TILE)
                k = k_of(sl)
                v = v_of(sl)
                k0, k1 = halves(k, factor)
                s0 = dot_nt(own_q2[0, ts, sl], k)
                s1 = dot_nt(own_q2[1, ts, sl], k)
                vd = dot_nt(own_g[ts, sl], v)
                aux = col_a[ts, :]
                p0 = jnp.exp2(s0 * LOG2E - aux[:, 4 * h : 4 * h + 1])
                p1 = jnp.exp2(s1 * LOG2E - aux[:, 4 * h + 1 : 4 * h + 2])
                if diagonal:
                    tpos = i * TILE + lax.broadcasted_iota(jnp.int32, (TILE, rows), 0)
                    spos = lax.broadcasted_iota(jnp.int32, (TILE, rows), 1)
                    vis = spos <= tpos
                    p0 = jnp.where(vis, p0, 0.0)
                    p1 = jnp.where(vis, p1, 0.0)
                d0 = (p0 * (vd - aux[:, 4 * h + 2 : 4 * h + 3])).astype(BF16)
                d1 = (p1 * (aux[:, 4 * h + 3 : 4 * h + 4] - vd)).astype(BF16)
                dqt = dot_nn(d0, k0) + dot_nn(d1, k1)
                if diagonal:
                    dq_ref[ts, sl] = dqt
                else:
                    dq_ref[ts, sl] += dqt
                return carry

            lax.fori_loop(0, rows // TILE, tile, 0)

    key_side(
        lambda sl: q_ref[:, sl], lambda sl: own_g[:, sl], lambda r: own_a[r : r + 1, :], True
    )
    query_side(lambda sl: k_ref[:, sl], lambda sl: own_v[:, sl], True)

    def key_slot(src):
        key_side(
            lambda sl: qbuf[src, :, sl],
            lambda sl: gbuf[src, :, sl],
            lambda r: abuf[src, r : r + 1, :],
            False,
        )

    def query_slot(src):
        query_side(lambda sl: kbuf[src, :, sl], lambda sl: vbuf[src, :, sl], False)

    def step(s, carry):
        up_own = pos - (s + 1)
        down_own = pos + (s + 1)
        up_src = 2 * up_own + col
        down_src = 2 * down_own + col
        has_up = up_own >= 0
        has_down = down_own < chain
        up_side = 2 * (pos - s) + 1 - col
        down_side = 2 * (pos + s) + 1 - col
        side_up = jnp.logical_and(pos - s >= 0, jnp.logical_or(s > 0, col == 1))
        side_down = jnp.logical_and(pos + s < chain, jnp.logical_or(s > 0, col == 0))

        @pl.when(has_down)
        def _():
            for stream in (qs, gs, as_):
                stream.wait(down_src)
                stream.forward(down_src, "start")

        @pl.when(has_up)
        def _():
            ks.wait(up_src)
            ks.forward(up_src, "start")

        @pl.when(side_down)
        def _():
            for stream in (qs, gs, as_):
                stream.wait(down_side)
            key_slot(down_side)

        @pl.when(has_up)
        def _():
            vs.wait(up_src)
            vs.forward(up_src, "start")

        @pl.when(has_down)
        def _():
            key_slot(down_src)

        @pl.when(side_up)
        def _():
            ks.wait(up_side)
            vs.wait(up_side)
            query_slot(up_side)

        @pl.when(has_up)
        def _():
            query_slot(up_src)

        return carry

    lax.fori_loop(0, chain, step, 0)

    narrow = dv_ref[...].astype(BF16)
    part[pl.ds(pl.multiple_of(tp * local, local), local), :] = dot_tn(
        lat_ref[...], narrow
    ).astype(BF16)

    def add_part(i, carry):
        @pl.when(i != tp)
        def _():
            part[pl.ds(pl.multiple_of(i * local, local), local), :] = dot_tn(
                lbuf[i], dv_ref[...].astype(BF16)
            ).astype(BF16)

        return carry

    lax.fori_loop(0, tp_n, add_part, 0)

    block = dw_ref.shape[0]

    def w_copy(dst):
        return rc(
            part.at[pl.ds(pl.multiple_of(dst * block, block), block)],
            wbuf.at[me],
            w_send.at[dst],
            w_recv.at[me],
            (dst, tp),
        )

    def w_wait(src):
        rc(
            part.at[pl.ds(0, block)], wbuf.at[src], w_send.at[src], w_recv.at[src], (src, tp)
        ).wait_recv()

    def w_start(i, carry):
        w_copy((me + i) % n).start()
        return carry

    lax.fori_loop(1, n, w_start, 0)
    dw_ref[...] = part[pl.ds(pl.multiple_of(me * block, block), block), :].astype(F32)

    def w_add(i, carry):
        src = (me + n - i) % n
        w_wait(src)
        dw_ref[...] += wbuf[src].astype(F32)
        return carry

    lax.fori_loop(1, n, w_add, 0)

    def w_done(i, carry):
        w_copy((me + i) % n).wait_send()
        return carry

    lax.fori_loop(1, n, w_done, 0)

    for stream in (qs, ks, gs, as_, vs):
        stream.send_own("wait_send")

    def drain(s, carry):
        @pl.when(pos + s < chain)
        def _():
            for stream in (qs, gs, as_):
                stream.forward(2 * (pos + s) + col, "wait_send")

        @pl.when(pos - s >= 0)
        def _():
            for stream in (ks, vs):
                stream.forward(2 * (pos - s) + col, "wait_send")

        return carry

    lax.fori_loop(1, chain, drain, 0)
    lat_mate().wait_send()
    for y in range(pairs):

        @pl.when(y != pair)
        def _():
            lat_copy(tp, y).wait_send()
            lat_fwd(2 * y + core).wait_send()


def solution(mesh):
    n = mesh.shape["sp"]
    tp_n = mesh.shape["tp"]

    def step(q, k, lat, w, logs, pair, cot, lam, gain):
        rows, qcols = q.shape
        dmodel, vcols = w.shape
        block = dmodel // n
        vmem = pl.BlockSpec(memory_space=pltpu.VMEM)
        dma = pltpu.SemaphoreType.DMA
        return pl.pallas_call(
            functools.partial(kernel, n, tp_n),
            name="diff_backward",
            out_shape=(
                jax.ShapeDtypeStruct((rows, qcols), F32),
                jax.ShapeDtypeStruct((rows, qcols), F32),
                jax.ShapeDtypeStruct((rows, vcols), F32),
                jax.ShapeDtypeStruct((block, vcols), F32),
            ),
            in_specs=[vmem] * 7 + [pl.BlockSpec(memory_space=pltpu.SMEM), vmem],
            out_specs=(vmem,) * 4,
            scratch_shapes=[
                pltpu.VMEM((n, rows, qcols), BF16),
                pltpu.VMEM((n, rows, vcols), BF16),
                pltpu.VMEM((n, rows, qcols), BF16),
                pltpu.VMEM((n, rows, vcols), BF16),
                pltpu.VMEM((n, 8, rows), F32),
                pltpu.VMEM((tp_n,) + lat.shape, BF16),
                pltpu.VMEM((rows, vcols), BF16),
                pltpu.VMEM((rows, vcols), BF16),
                pltpu.VMEM((8, rows), F32),
                pltpu.VMEM((rows, 128), F32),
                pltpu.VMEM((2, rows, qcols), BF16),
                pltpu.VMEM((2, rows, qcols), BF16),
                pltpu.VMEM((dmodel, vcols), BF16),
                pltpu.VMEM((n, block, vcols), BF16),
                dma((tp_n // 2,)),
                dma((tp_n,)),
                dma((tp_n,)),
                dma((tp_n,)),
                dma((2, n)),
                dma((n,)),
                dma((2, n)),
                dma((n,)),
                dma((2, n)),
                dma((n,)),
                dma((2, n)),
                dma((n,)),
                dma((2, n)),
                dma((n,)),
                dma((n,)),
                dma((n,)),
            ],
            compiler_params=pltpu.CompilerParams(
                collective_id=0, has_side_effects=True, vmem_limit_bytes=60 * 1024 * 1024
            ),
        )(q, k, lat, w, logs, pair, cot, lam, gain.reshape(1, -1))

    return jax.shard_map(
        step,
        mesh=mesh,
        in_specs=(
            P("sp", "tp"),
            P("sp", "tp"),
            P("sp", "tp"),
            P(None, "tp"),
            P("sp", "tp"),
            P("sp", "tp"),
            P("sp", "tp"),
            P("tp"),
            P(),
        ),
        out_specs=(P("sp", "tp"), P("sp", "tp"), P("sp", "tp"), P("sp", "tp")),
        check_vma=False,
    )
```

```python
import functools
import math

import jax
import jax.numpy as jnp
from jax import lax
from jax.experimental import pallas as pl
from jax.experimental.pallas import tpu as pltpu
from jax.sharding import PartitionSpec as P

MESH = pl.DeviceIdType.MESH
F32 = jnp.float32
BF16 = jnp.bfloat16
LOG2E = math.log2(math.e)
norm_floor = 0.25
TILE = 256


def dot_nn(a, b):
    return lax.dot_general(a, b, (((1,), (0,)), ((), ())), preferred_element_type=F32)


def dot_nt(a, b):
    return lax.dot_general(a, b, (((1,), (1,)), ((), ())), preferred_element_type=F32)


def dot_tn(a, b):
    return lax.dot_general(a, b, (((0,), (0,)), ((), ())), preferred_element_type=F32)


def halves(block, factor):
    width = block.shape[-1]
    lane = lax.broadcasted_iota(jnp.int32, block.shape, 1)
    wide = block.astype(F32) * factor
    return (
        jnp.where(lane < width // 2, wide, 0.0).astype(BF16),
        jnp.where(lane < width // 2, 0.0, wide).astype(BF16),
    )


def kernel(
    n,
    tp_n,
    q_ref,
    k_ref,
    lat_ref,
    w_ref,
    log_ref,
    pair_ref,
    cot_ref,
    lam_ref,
    gain_ref,
    dq_ref,
    dk_ref,
    dv_ref,
    dw_ref,
    kbuf,
    vbuf,
    qbuf,
    gbuf,
    abuf,
    lbuf,
    own_v,
    own_g,
    own_a,
    col_a,
    own_k2,
    own_q2,
    part,
    wbuf,
    lat_send,
    lat_recv,
    fwd_send,
    fwd_recv,
    k_send,
    k_recv,
    v_send,
    v_recv,
    q_send,
    q_recv,
    g_send,
    g_recv,
    a_send,
    a_recv,
    w_send,
    w_recv,
):
    heads = lam_ref.shape[0]
    rows = q_ref.shape[0]
    width = q_ref.shape[1] // heads
    me = lax.axis_index("sp")
    tp = lax.axis_index("tp")
    chain = n // 2
    pos = me // 2
    col = me % 2
    factor = (width // 2) ** (-0.5)

    barrier = pltpu.get_barrier_semaphore()

    def greet_sp(i, carry):
        @pl.when(i != me)
        def _():
            pl.semaphore_signal(barrier, inc=1, device_id=(i, tp), device_id_type=MESH)

        return carry

    def greet_tp(i, carry):
        @pl.when(i != tp)
        def _():
            pl.semaphore_signal(barrier, inc=1, device_id=(me, i), device_id_type=MESH)

        return carry

    lax.fori_loop(0, n, greet_sp, 0)
    lax.fori_loop(0, tp_n, greet_tp, 0)
    pl.semaphore_wait(barrier, n - 1 + tp_n - 1)

    core = tp % 2
    pair = tp // 2
    mate = 2 * pair + 1 - core
    pairs = tp_n // 2

    def rc(src, dst, ssem, rsem, dev):
        return pltpu.make_async_remote_copy(
            src_ref=src,
            dst_ref=dst,
            send_sem=ssem,
            recv_sem=rsem,
            device_id=dev,
            device_id_type=MESH,
        )

    def lat_copy(slot_src, y):
        return rc(
            lat_ref, lbuf.at[slot_src], lat_send.at[y], lat_recv.at[slot_src], (me, 2 * y + core)
        )

    def lat_mate():
        return rc(lat_ref, lbuf.at[tp], fwd_send.at[tp], fwd_recv.at[tp], (me, mate))

    def lat_fwd(src):
        return rc(lbuf.at[src], lbuf.at[src], fwd_send.at[src], fwd_recv.at[src], (me, mate))

    class Stream:
        def __init__(self, own, buf, ssem, rsem, step):
            self.own, self.buf, self.ssem, self.rsem, self.step = own, buf, ssem, rsem, step

        def onward(self):
            nxt = pos + self.step
            return jnp.logical_and(nxt >= 0, nxt < chain)

        def copy(self, h, src, ref, way):
            dev = (jnp.clip(me + 2 * self.step, 0, n - 1), 2 * pos + 1 - col)[way]
            return rc(
                ref,
                self.buf.at[h, src],
                self.ssem.at[h, way, src],
                self.rsem.at[h, src],
                (dev, tp),
            )

        def send_own(self, h, act):
            @pl.when(self.onward())
            def _():
                getattr(self.copy(h, me, self.own(h), 0), act)()

            @pl.when(col == (0 if self.step == 1 else 1))
            def _():
                getattr(self.copy(h, me, self.own(h), 1), act)()

        def forward(self, h, src, act):
            getattr(self.copy(h, src, self.buf.at[h, src], 1), act)()

            @pl.when(self.onward())
            def _():
                getattr(self.copy(h, src, self.buf.at[h, src], 0), act)()

        def wait(self, h, src):
            self.copy(h, src, self.buf.at[h, src], 0).wait_recv()

    def lanes(h):
        return slice(h * width, (h + 1) * width)

    ks = Stream(lambda h: k_ref.at[:, lanes(h)], kbuf, k_send, k_recv, 1)
    vs = Stream(lambda h: own_v.at[:, lanes(h)], vbuf, v_send, v_recv, 1)
    qs = Stream(lambda h: q_ref.at[:, lanes(h)], qbuf, q_send, q_recv, -1)
    gs = Stream(lambda h: own_g.at[:, lanes(h)], gbuf, g_send, g_recv, -1)
    as_ = Stream(lambda h: own_a.at[h], abuf, a_send, a_recv, -1)

    for y in range(pairs):

        @pl.when(y != pair)
        def _():
            lat_copy(tp, y).start()

    lat_mate().start()
    qs.send_own(0, "start")
    ks.send_own(0, "start")

    lane = lax.broadcasted_iota(jnp.int32, (rows, 128), 1)
    packed = jnp.zeros((rows, 128), F32)
    log_rows = log_ref.shape[0]
    log_cols = jnp.transpose(
        jnp.concatenate([log_ref[...], jnp.zeros((128 - log_rows, rows), F32)], axis=0)
    )
    for h in range(heads):
        lam = lam_ref[h]
        a = pair_ref[:, (2 * h) * width : (2 * h + 1) * width].astype(F32)
        b = pair_ref[:, (2 * h + 1) * width : (2 * h + 2) * width].astype(F32)
        merged = a - lam * b
        inv = lax.rsqrt(jnp.mean(merged * merged, axis=-1, keepdims=True) + norm_floor)
        g = cot_ref[:, h * width : (h + 1) * width].astype(F32) * gain_ref[...]
        inner = jnp.mean(g * merged, axis=-1, keepdims=True)
        og = (inv * g - merged * (inv * inv * inv) * inner).astype(BF16)
        own_g[:, h * width : (h + 1) * width] = og
        wide = og.astype(F32)
        first = jnp.sum(wide * a, axis=-1, keepdims=True)
        second = jnp.sum(wide * b, axis=-1, keepdims=True)
        log_lam = jnp.log(jnp.full((1, 128), lam, F32))
        log0 = log_cols[:, 2 * h : 2 * h + 1] * LOG2E
        log1 = (log_cols[:, 2 * h + 1 : 2 * h + 2] - log_lam) * LOG2E
        packed = jnp.where(lane == 4 * h, log0, packed)
        packed = jnp.where(lane == 4 * h + 1, log1, packed)
        packed = jnp.where(lane == 4 * h + 2, first, packed)
        packed = jnp.where(lane == 4 * h + 3, second, packed)
    col_a[...] = packed
    flipped = jnp.transpose(packed)
    for h in range(heads):
        own_a[h, 0:4, :] = flipped[4 * h : 4 * h + 4, :]
        own_a[h, 4:8, :] = jnp.zeros((4, rows), F32)
    gs.send_own(0, "start")
    as_.send_own(0, "start")

    for h in range(heads):
        sl = slice(h * width, (h + 1) * width)
        k0, k1 = halves(k_ref[:, sl], factor)
        own_k2[0, :, sl] = k0
        own_k2[1, :, sl] = k1
        q0, q1 = halves(q_ref[:, sl], factor)
        own_q2[0, :, sl] = q0
        own_q2[1, :, sl] = q1

    def pass_down(h, s):
        src = 2 * (pos + s) + col

        @pl.when(pos + s < chain)
        def _():
            for stream in (qs, gs, as_):
                stream.wait(h, src)
                stream.forward(h, src, "start")

    def pass_keys(h, s):
        src = 2 * (pos - s) + col

        @pl.when(pos - s >= 0)
        def _():
            ks.wait(h, src)
            ks.forward(h, src, "start")

    pass_down(0, 1)
    pass_keys(0, 1)

    local = w_ref.shape[0] // tp_n

    def spread_latents():
        for y in range(pairs):

            @pl.when(y != pair)
            def _():
                src = 2 * y + core
                lat_copy(src, y).wait_recv()
                lat_fwd(src).start()

    def make_values():
        for y in range(pairs):
            lat_fwd(2 * y + 1 - core).wait_recv()
        lbuf[tp] = lat_ref[...]
        total = dot_nn(lbuf[0], w_ref[0:local, :])
        for i in range(1, tp_n):
            total += dot_nn(lbuf[i], w_ref[i * local : (i + 1) * local, :])
        own_v[...] = total.astype(BF16)
        vs.send_own(0, "start")

    def key_side(h, q_of, g_of, a_of, diagonal):
        sl = lanes(h)

        def tile(i, carry):
            ts = pl.ds(pl.multiple_of(i * TILE, TILE), TILE)
            q = q_of()
            g = g_of()
            q0, q1 = halves(q, factor)
            s0 = dot_nt(own_k2[0, ts, sl], q)
            s1 = dot_nt(own_k2[1, ts, sl], q)
            vd = dot_nt(own_v[ts, sl], g)
            p0 = jnp.exp2(s0 * LOG2E - a_of(0))
            p1 = jnp.exp2(s1 * LOG2E - a_of(1))
            if diagonal:
                spos = i * TILE + lax.broadcasted_iota(jnp.int32, (TILE, rows), 0)
                tpos = lax.broadcasted_iota(jnp.int32, (TILE, rows), 1)
                vis = spos <= tpos
                p0 = jnp.where(vis, p0, 0.0)
                p1 = jnp.where(vis, p1, 0.0)
            mixed = (p0 - p1).astype(BF16)
            d0 = (p0 * (vd - a_of(2))).astype(BF16)
            d1 = (p1 * (a_of(3) - vd)).astype(BF16)
            dvt = dot_nn(mixed, g)
            dkt = dot_nn(d0, q0) + dot_nn(d1, q1)
            if diagonal:
                dv_ref[ts, sl] = dvt
                dk_ref[ts, sl] = dkt
            else:
                dv_ref[ts, sl] += dvt
                dk_ref[ts, sl] += dkt
            return carry

        lax.fori_loop(0, rows // TILE, tile, 0)

    def query_side(h, k_of, v_of, diagonal):
        sl = lanes(h)

        def tile(i, carry):
            ts = pl.ds(pl.multiple_of(i * TILE, TILE), TILE)
            k = k_of()
            v = v_of()
            k0, k1 = halves(k, factor)
            s0 = dot_nt(own_q2[0, ts, sl], k)
            s1 = dot_nt(own_q2[1, ts, sl], k)
            vd = dot_nt(own_g[ts, sl], v)
            aux = col_a[ts, :]
            p0 = jnp.exp2(s0 * LOG2E - aux[:, 4 * h : 4 * h + 1])
            p1 = jnp.exp2(s1 * LOG2E - aux[:, 4 * h + 1 : 4 * h + 2])
            if diagonal:
                tpos = i * TILE + lax.broadcasted_iota(jnp.int32, (TILE, rows), 0)
                spos = lax.broadcasted_iota(jnp.int32, (TILE, rows), 1)
                vis = spos <= tpos
                p0 = jnp.where(vis, p0, 0.0)
                p1 = jnp.where(vis, p1, 0.0)
            d0 = (p0 * (vd - aux[:, 4 * h + 2 : 4 * h + 3])).astype(BF16)
            d1 = (p1 * (aux[:, 4 * h + 3 : 4 * h + 4] - vd)).astype(BF16)
            dqt = dot_nn(d0, k0) + dot_nn(d1, k1)
            if diagonal:
                dq_ref[ts, sl] = dqt
            else:
                dq_ref[ts, sl] += dqt
            return carry

        lax.fori_loop(0, rows // TILE, tile, 0)

    block = dw_ref.shape[0]

    def w_copy(h, dst):
        return rc(
            part.at[h, pl.ds(pl.multiple_of(dst * block, block), block)],
            wbuf.at[h, me],
            w_send.at[h, dst],
            w_recv.at[h, me],
            (dst, tp),
        )

    def w_wait(h, src):
        rc(
            part.at[h, pl.ds(0, block)],
            wbuf.at[h, src],
            w_send.at[h, src],
            w_recv.at[h, src],
            (src, tp),
        ).wait_recv()

    def weight_partials(h):
        per = local // block

        def one_slot(i, carry):
            slot = tp_n - 1 - i
            part[h, pl.ds(pl.multiple_of(slot * local, local), local), :] = dot_tn(
                lbuf[slot], dv_ref[:, lanes(h)].astype(BF16)
            ).astype(BF16)
            for r in range(per):
                dst = slot * per + per - 1 - r

                @pl.when(dst != me)
                def _():
                    w_copy(h, dst).start()

            return carry

        lax.fori_loop(0, tp_n, one_slot, 0)

    def key_slot(h, src):
        key_side(
            h,
            lambda: qbuf[h, src],
            lambda: gbuf[h, src],
            lambda r: abuf[h, src, r : r + 1, :],
            False,
        )

    def query_slot(h, src):
        query_side(h, lambda: kbuf[h, src], lambda: vbuf[h, src], False)

    def run_head(h):
        sl = lanes(h)
        more = h + 1 < heads
        lag = 2 if h == 0 else 0
        vlag = 2 if h == 0 else 1
        total_steps = chain + vlag + 1
        if h == 0 and more:
            total_steps = max(total_steps, 2 * chain - 1)

        def step(s, carry):
            if h == 0:

                @pl.when(s > 0)
                def _():
                    pass_down(h, s + 1)
                    pass_keys(h, s + 1)

                @pl.when(s == 1)
                def _():
                    spread_latents()

            if more:

                @pl.when(s == 0)
                def _():
                    for stream in (qs, gs, as_):
                        stream.send_own(h + 1, "start")

                @pl.when(s == pos)
                def _():
                    ks.send_own(h + 1, "start")

                @pl.when(s > chain - 1 - pos)
                def _():
                    pass_down(h + 1, s - (chain - 1 - pos))

                @pl.when(s > pos)
                def _():
                    pass_keys(h + 1, s - pos)

            if h == 0:

                @pl.when(s == 2)
                def _():
                    make_values()

            if more:

                @pl.when(s == jnp.maximum(pos, 2))
                def _():
                    vs.send_own(h + 1, "start")

            @pl.when(s == lag)
            def _():
                key_side(
                    h,
                    lambda: q_ref[:, sl],
                    lambda: own_g[:, sl],
                    lambda r: own_a[h, r : r + 1, :],
                    True,
                )

            up = s - vlag
            up_own = pos - up
            has_up = jnp.logical_and(up_own >= 0, up >= 1)

            @pl.when(has_up)
            def _():
                vs.wait(h, 2 * up_own + col)
                vs.forward(h, 2 * up_own + col, "start")

            far = s - lag
            down_side = 2 * (pos + far) + 1 - col
            side_down = jnp.logical_and(
                jnp.logical_and(pos + far < chain, far >= 0), jnp.logical_or(far > 0, col == 0)
            )

            @pl.when(jnp.logical_and(pos + far + 1 < chain, far >= 0))
            def _():
                key_slot(h, 2 * (pos + far + 1) + col)

            @pl.when(side_down)
            def _():
                for stream in (qs, gs, as_):
                    stream.wait(h, down_side)
                key_slot(h, down_side)

            @pl.when(far == chain - 1)
            def _():
                weight_partials(h)

            @pl.when(s == lag)
            def _():
                query_side(h, lambda: k_ref[:, sl], lambda: own_v[:, sl], True)

            @pl.when(has_up)
            def _():
                query_slot(h, 2 * up_own + col)

            side = up - 1
            up_side = 2 * (pos - side) + 1 - col
            side_up = jnp.logical_and(
                jnp.logical_and(pos - side >= 0, side >= 0), jnp.logical_or(side > 0, col == 1)
            )

            @pl.when(side_up)
            def _():
                ks.wait(h, up_side)
                vs.wait(h, up_side)
                query_slot(h, up_side)

            return carry

        lax.fori_loop(0, total_steps, step, 0)

    if heads > 2:
        raise NotImplementedError
    for h in range(heads):
        run_head(h)

    own_rows = pl.ds(pl.multiple_of(me * block, block), block)
    for h in range(heads):
        dw_ref[:, lanes(h)] = part[h, own_rows, :].astype(F32)

        def w_add(i, carry):
            src = (me + n - i) % n
            w_wait(h, src)
            dw_ref[:, lanes(h)] += wbuf[h, src].astype(F32)
            return carry

        lax.fori_loop(1, n, w_add, 0)

    for h in range(heads):

        def w_done(i, carry):
            w_copy(h, (me + i) % n).wait_send()
            return carry

        lax.fori_loop(1, n, w_done, 0)

        for stream in (qs, ks, gs, as_, vs):
            stream.send_own(h, "wait_send")

        def drain(s, carry):
            @pl.when(pos + s < chain)
            def _():
                for stream in (qs, gs, as_):
                    stream.forward(h, 2 * (pos + s) + col, "wait_send")

            @pl.when(pos - s >= 0)
            def _():
                for stream in (ks, vs):
                    stream.forward(h, 2 * (pos - s) + col, "wait_send")

            return carry

        lax.fori_loop(1, chain, drain, 0)

    lat_mate().wait_send()
    for y in range(pairs):

        @pl.when(y != pair)
        def _():
            lat_copy(tp, y).wait_send()
            lat_fwd(2 * y + core).wait_send()


def solution(mesh):
    n = mesh.shape["sp"]
    tp_n = mesh.shape["tp"]

    def step(q, k, lat, w, logs, pair, cot, lam, gain):
        rows, qcols = q.shape
        dmodel, vcols = w.shape
        block = dmodel // n
        heads = lam.shape[0]
        width = vcols // heads
        vmem = pl.BlockSpec(memory_space=pltpu.VMEM)
        dma = pltpu.SemaphoreType.DMA
        return pl.pallas_call(
            functools.partial(kernel, n, tp_n),
            name="diff_backward",
            out_shape=(
                jax.ShapeDtypeStruct((rows, qcols), F32),
                jax.ShapeDtypeStruct((rows, qcols), F32),
                jax.ShapeDtypeStruct((rows, vcols), F32),
                jax.ShapeDtypeStruct((block, vcols), F32),
            ),
            in_specs=[vmem] * 7 + [pl.BlockSpec(memory_space=pltpu.SMEM), vmem],
            out_specs=(vmem,) * 4,
            scratch_shapes=[
                pltpu.VMEM((heads, n, rows, width), BF16),
                pltpu.VMEM((heads, n, rows, width), BF16),
                pltpu.VMEM((heads, n, rows, width), BF16),
                pltpu.VMEM((heads, n, rows, width), BF16),
                pltpu.VMEM((heads, n, 8, rows), F32),
                pltpu.VMEM((tp_n,) + lat.shape, BF16),
                pltpu.VMEM((rows, vcols), BF16),
                pltpu.VMEM((rows, vcols), BF16),
                pltpu.VMEM((heads, 8, rows), F32),
                pltpu.VMEM((rows, 128), F32),
                pltpu.VMEM((2, rows, qcols), BF16),
                pltpu.VMEM((2, rows, qcols), BF16),
                pltpu.VMEM((heads, dmodel, width), BF16),
                pltpu.VMEM((heads, n, block, width), BF16),
                dma((tp_n // 2,)),
                dma((tp_n,)),
                dma((tp_n,)),
                dma((tp_n,)),
                dma((heads, 2, n)),
                dma((heads, n)),
                dma((heads, 2, n)),
                dma((heads, n)),
                dma((heads, 2, n)),
                dma((heads, n)),
                dma((heads, 2, n)),
                dma((heads, n)),
                dma((heads, 2, n)),
                dma((heads, n)),
                dma((heads, n)),
                dma((heads, n)),
            ],
            compiler_params=pltpu.CompilerParams(
                collective_id=0, has_side_effects=True, vmem_limit_bytes=60 * 1024 * 1024
            ),
        )(q, k, lat, w, logs.T, pair, cot, lam, gain.reshape(1, -1))

    return jax.shard_map(
        step,
        mesh=mesh,
        in_specs=(
            P("sp", "tp"),
            P("sp", "tp"),
            P("sp", "tp"),
            P(None, "tp"),
            P("sp", "tp"),
            P("sp", "tp"),
            P("sp", "tp"),
            P("tp"),
            P(),
        ),
        out_specs=(P("sp", "tp"), P("sp", "tp"), P("sp", "tp"), P("sp", "tp")),
        check_vma=False,
    )
```
